32 devices in a mesh: fs: 8 (over z, y), tp: 4 (over x, core).
Axes of the slice: x: 2, y: 2, z: 4, core: 2. Of those that a mesh axis runs over, the one named last changes fastest.
Arguments:
- tokens: bfloat16 [2048, 2048], P('fs', 'tp'), may hold values from -12.1 to 12.1, as said below
- gate_weight: float32 [2048, 5632], P('fs', 'tp'), may hold values from -0.125 to 0.125
- up_weight: float32 [2048, 5632], P('fs', 'tp'), may hold values from -0.125 to 0.125
- down_weight: float32 [5632, 2048], P('tp', 'fs'), may hold values from -0.078125 to 0.078125
- gate_scale: float32 [4, 1408], P('tp', 'fs'), may hold values from 0.1 to 1.9
- up_scale: float32 [4, 1408], P('tp', 'fs'), may hold values from 0.1 to 1.9
- down_scale: float32 [4, 512], P('tp', 'fs'), may hold values from 0.16 to 4.6, as said below
- bgate_weight: float32 [2048, 2048], P('fs', 'tp'), may hold values from -0.125 to 0.125
- cgate_weight: float32 [2048, 2048], P('fs', 'tp'), may hold values from -0.125 to 0.125
- value_weight: float32 [2048, 2048], P('fs', 'tp'), may hold values from -0.125 to 0.125
- bgate_scale: float32 [4, 512], P('tp', 'fs'), may hold values from 0.1 to 1.9
- cgate_scale: float32 [4, 512], P('tp', 'fs'), may hold values from 0.1 to 1.9
- value_scale: float32 [4, 512], P('tp', 'fs'), may hold values from 0.1 to 1.9
- conv_taps: float32 [3, 2048], replicated, may hold values from -3.5 to 3.5
- mixout_weight: float32 [2048, 2048], P('tp', 'fs'), may hold values from -0.125 to 0.125
- mixout_scale: float32 [4, 512], P('tp', 'fs'), may hold values from 0.16 to 4.6, as said below
- first_gain: float32 [2048], replicated, may hold values from 0.1 to 1.9
- first_shift: float32 [2048], replicated, may hold values from -1.8 to 1.8
- mixer_gain: float32 [2048], replicated, may hold values from 0.1 to 1.9
- mixer_shift: float32 [2048], replicated, may hold values from -1.8 to 1.8
- last_gain: float32 [2048], replicated, may hold values from 0.1 to 1.9
- last_shift: float32 [2048], replicated, may hold values from -1.8 to 1.8
Outputs:
- layer_out: bfloat16 [2048, 2048], P('fs', 'tp')
The draws below stay inside these ranges and needn't reach their ends.
Inputs may be any that keep to these rules, and one draw needn't show every extreme that they name: `tokens`: normal values times one factor for each of 4 equal consecutive blocks of the features. `down_scale`: positive; one factor for each row times a spread over the columns. `mixout_scale`: positive; one factor for each row times a spread over the columns.
All inputs are finite; a program needn't handle non-finite values.
Results may differ from the reference program's by a relative error of at most 0.025.
Values may be sent and summed in bfloat16 or wider, within the bound.
No kernel may reach another device: no remote copies, remote signals or barrier semaphores. Data moves between devices by JAX's collectives and lax.ppermute only.
A program may use at most 64 MiB of HBM per device.

```python
import jax
import jax.numpy as jnp
from jax import lax

D = 2048
FF = 5632
CONV_CH = 2048
TAPS = 3
LENGTH = 128
TOKENS = 2048
N_TP = 4


def block_factors(key, blocks):
    return jnp.exp(jax.random.uniform(key, (blocks, 1), jnp.float32, -1.1, 1.1))


def draw_tokens(key, part):
    values = jnp.clip(jax.random.normal(jax.random.fold_in(key, 11), (TOKENS, D), jnp.float32), -4.0, 4.0)
    factor = block_factors(jax.random.fold_in(key, 12), N_TP)
    column_factor = jnp.repeat(factor[:, 0], D // N_TP)
    return (values * column_factor[None, :]).astype(jnp.bfloat16)


def column_scale(key):
    factor = block_factors(jax.random.fold_in(key, 1), N_TP)
    spread_part = jax.random.uniform(jax.random.fold_in(key, 2), (N_TP, D // N_TP), jnp.float32, 0.7, 1.3)
    return factor * spread_part


def draw_down_scale(key, part):
    return column_scale(jax.random.fold_in(key, 21))


def draw_mixout_scale(key, part):
    return column_scale(jax.random.fold_in(key, 22))


def block_levels(stream_key, dims, split, smallest, high):
    factor_of, own = 1.0, jax.random.fold_in(stream_key, 6)
    for axis_at, blocks in split:
        draws = jnp.exp(jax.random.uniform(jax.random.fold_in(own, axis_at), (blocks,), jnp.float32, smallest / len(split), high / len(split)))
        factor_of = factor_of * jnp.repeat(draws, dims[axis_at] // blocks).reshape([-1 if axis == axis_at else 1 for axis in range(len(dims))])
    return factor_of


def scatter_about(key, shape, scale, bound, cuts=(), held_as=jnp.bfloat16):
    values = scale * jax.random.normal(key, shape, jnp.float32)
    if cuts:
        values = values * block_levels(key, shape, cuts, -0.22, 0.18)
    return jnp.clip(values, -bound, bound).astype(held_as)


def setup_inputs(seed: int = 0) -> dict:
    key_list = jax.random.split(jax.random.key(seed), 23)
    return {
        "tokens": draw_tokens(jax.random.fold_in(key_list[22], 71), 0),
        "gate_weight": scatter_about(key_list[1], (D, FF), D ** -0.5, 0.125, ((0, 8), (1, 4)), jnp.float32),
        "up_weight": scatter_about(key_list[2], (D, FF), D ** -0.5, 0.125, ((0, 8), (1, 4)), jnp.float32),
        "down_weight": scatter_about(key_list[3], (FF, D), FF ** -0.5, 0.078125, ((0, 4), (1, 8)), jnp.float32),
        "gate_scale": jnp.clip(1.0 + 0.18 * jax.random.normal(key_list[4], (N_TP, FF // N_TP), jnp.float32), 0.1, 1.9),
        "up_scale": jnp.clip(1.0 + 0.18 * jax.random.normal(key_list[5], (N_TP, FF // N_TP), jnp.float32), 0.1, 1.9),
        "down_scale": draw_down_scale(jax.random.fold_in(key_list[22], 71), 0),
        "bgate_weight": scatter_about(key_list[7], (D, CONV_CH), D ** -0.5, 0.125, ((0, 8), (1, 4)), jnp.float32),
        "cgate_weight": scatter_about(key_list[8], (D, CONV_CH), D ** -0.5, 0.125, ((0, 8), (1, 4)), jnp.float32),
        "value_weight": scatter_about(key_list[9], (D, CONV_CH), D ** -0.5, 0.125, ((0, 8), (1, 4)), jnp.float32),
        "bgate_scale": jnp.clip(1.0 + 0.18 * jax.random.normal(key_list[10], (N_TP, CONV_CH // N_TP), jnp.float32), 0.1, 1.9),
        "cgate_scale": jnp.clip(1.0 + 0.18 * jax.random.normal(key_list[11], (N_TP, CONV_CH // N_TP), jnp.float32), 0.1, 1.9),
        "value_scale": jnp.clip(1.0 + 0.18 * jax.random.normal(key_list[12], (N_TP, CONV_CH // N_TP), jnp.float32), 0.1, 1.9),
        "conv_taps": scatter_about(key_list[13], (TAPS, CONV_CH), TAPS ** -0.5, 3.5, (), jnp.float32),
        "mixout_weight": scatter_about(key_list[14], (CONV_CH, D), CONV_CH ** -0.5, 0.125, ((0, 4), (1, 8)), jnp.float32),
        "mixout_scale": draw_mixout_scale(jax.random.fold_in(key_list[22], 71), 0),
        "first_gain": jnp.clip(1.0 + 0.18 * jax.random.normal(key_list[16], (D,), jnp.float32), 0.1, 1.9),
        "first_shift": scatter_about(key_list[17], (D,), 0.3, 1.8, (), jnp.float32),
        "mixer_gain": jnp.clip(1.0 + 0.18 * jax.random.normal(key_list[18], (D,), jnp.float32), 0.1, 1.9),
        "mixer_shift": scatter_about(key_list[19], (D,), 0.3, 1.8, (), jnp.float32),
        "last_gain": jnp.clip(1.0 + 0.18 * jax.random.normal(key_list[20], (D,), jnp.float32), 0.1, 1.9),
        "last_shift": scatter_about(key_list[21], (D,), 0.3, 1.8, (), jnp.float32),
    }


RESIDUAL_SCALE = 1.4142135623730951
HALF_STEP = 0.5
EPSILON = 1e-05

def post_norm(residual, branch, norm_gain, norm_shift):
    summed = RESIDUAL_SCALE * residual.astype(jnp.float32) + branch
    average = lax.optimization_barrier(jnp.mean(summed, -1, keepdims=True))
    mean_square = lax.optimization_barrier(jnp.mean(summed * summed, -1, keepdims=True))
    variance = mean_square - average * average
    return ((summed - average) * lax.rsqrt(variance + EPSILON) * norm_gain + norm_shift).astype(jnp.bfloat16)

def block_sum(left_rows, right_cols):
    block_width = left_rows.shape[1] // N_TP
    running = jnp.zeros((left_rows.shape[0], right_cols.shape[1]), jnp.float32)
    for block_index in range(N_TP):
        low = block_index * block_width
        partial_value = jnp.dot(left_rows[:, low:low + block_width], right_cols[low:low + block_width], preferred_element_type=jnp.float32)
        running = running + lax.optimization_barrier(partial_value.astype(jnp.bfloat16)).astype(jnp.float32)
    return running

def scaled_dot(inputs, matrix, scales):
    product = jnp.dot(inputs, matrix.astype(jnp.bfloat16), preferred_element_type=jnp.float32)
    return product * scales.reshape(-1)

def feed(inputs, gate_weight, up_weight, down_weight, gate_scale, up_scale, down_scale):
    gate_sum = scaled_dot(inputs, gate_weight, gate_scale)
    up_sum = scaled_dot(inputs, up_weight, up_scale)
    hidden = (jax.nn.silu(gate_sum) * up_sum).astype(jnp.bfloat16)
    result = block_sum(hidden, down_weight.astype(jnp.bfloat16)) * down_scale.reshape(-1)
    return HALF_STEP * result

def causal_conv(mixed, conv_taps):
    channels = mixed.shape[1]
    shaped = mixed.reshape(-1, LENGTH, channels)
    padded = jnp.pad(shaped, ((0, 0), (TAPS - 1, 0), (0, 0)))
    convolved = jnp.zeros(shaped.shape, jnp.float32)
    for tap_index in range(TAPS):
        convolved = convolved + conv_taps[tap_index] * padded[:, tap_index:tap_index + LENGTH]
    return convolved.reshape(-1, channels)

def reference(tokens, gate_weight, up_weight, down_weight, gate_scale, up_scale, down_scale, bgate_weight, cgate_weight, value_weight, bgate_scale, cgate_scale, value_scale, conv_taps, mixout_weight, mixout_scale, first_gain, first_shift, mixer_gain, mixer_shift, last_gain, last_shift):
    ffn_args = (gate_weight, up_weight, down_weight, gate_scale, up_scale, down_scale)
    first = post_norm(tokens, feed(tokens, *ffn_args), first_gain, first_shift)
    outgate = scaled_dot(first, bgate_weight, bgate_scale)
    ingate = scaled_dot(first, cgate_weight, cgate_scale)
    values = scaled_dot(first, value_weight, value_scale)
    convolved = causal_conv(ingate * values, conv_taps)
    gated = (outgate * convolved).astype(jnp.bfloat16)
    token_mix = block_sum(gated, mixout_weight.astype(jnp.bfloat16)) * mixout_scale.reshape(-1)
    second = post_norm(first, token_mix, mixer_gain, mixer_shift)
    return post_norm(second, feed(second, *ffn_args), last_gain, last_shift)
```

```python
import jax
import jax.numpy as jnp
from jax import lax
from jax.sharding import PartitionSpec as P

TAPS = 3
LENGTH = 128
RESIDUAL_SCALE = 1.4142135623730951
HALF_STEP = 0.5
EPSILON = 1e-05
AXES = ("fs", "tp")
DIMS = ("zh", "zl", "y", "x", "c")


class Layout:
    def __init__(self, mesh):
        fs, tp = mesh.shape["fs"], mesh.shape["tp"]
        cores = 2 if tp % 2 == 0 else 1
        nx = tp // cores
        ny = nx if fs % nx == 0 else 1
        nz = fs // ny
        nl = 2 if nz % 2 == 0 else 1
        self.size = {"zh": nz // nl, "zl": nl, "y": ny, "x": nx, "c": cores}
        self.fs, self.tp = fs, tp

    def flat(self, at):
        s = self.size
        fs = (at["zh"] * s["zl"] + at["zl"]) * s["y"] + at["y"]
        return fs * self.tp + at["x"] * s["c"] + at["c"]

    def coords(self):
        points = [{}]
        for dim in DIMS:
            points = [dict(p, **{dim: i}) for p in points for i in range(self.size[dim])]
        return points

    def here(self):
        s = self.size
        fs, tp = lax.axis_index("fs"), lax.axis_index("tp")
        return {
            "zh": fs // (s["y"] * s["zl"]),
            "zl": (fs // s["y"]) % s["zl"],
            "y": fs % s["y"],
            "x": tp // s["c"],
            "c": tp % s["c"],
        }

    def send(self, value, **shift):
        pairs = []
        for at in self.coords():
            to = {d: (at[d] + shift.get(d, 0)) % self.size[d] for d in DIMS}
            pairs.append((self.flat(at), self.flat(to)))
        return lax.ppermute(value, AXES, pairs)

    def back(self, here, dim, step):
        return (here[dim] + self.size[dim] - step) % self.size[dim]


def pick(stack, index):
    return lax.dynamic_index_in_dim(stack, index, 0, keepdims=False)


def gather_small(lay, here, value):
    for dim in ("c", "x", "y", "zl", "zh"):
        size = lay.size[dim]
        out = jnp.zeros((size,) + value.shape, value.dtype)
        out = lax.dynamic_update_index_in_dim(out, value, here[dim], 0)
        for step in range(1, size):
            got = lay.send(value, **{dim: step})
            out = lax.dynamic_update_index_in_dim(out, got, lay.back(here, dim, step), 0)
        value = out
    return value.reshape(lay.fs, lay.tp, -1)


def gather_pieces(lay, here, halves):
    s = lay.size
    pieces = [(here["zh"], here["zl"], here["y"], pick(halves, here["zl"]))]
    for step in range(1, s["zl"]):
        part = pick(halves, (here["zl"] + step) % s["zl"])
        pieces.append((here["zh"], lay.back(here, "zl", step), here["y"], lay.send(part, zl=step)))
    for zh, zl, y, part in list(pieces):
        for step in range(1, s["zh"]):
            pieces.append((lay.back(here, "zh", step), zl, y, lay.send(part, zh=step)))
    for zh, zl, y, part in list(pieces):
        for step in range(1, s["y"]):
            pieces.append((zh, zl, lay.back(here, "y", step), lay.send(part, y=step)))
    return [((zh * s["zl"] + zl) * s["y"] + y, part) for zh, zl, y, part in pieces]


def assemble(pieces, count):
    out = jnp.zeros((count,) + pieces[0][1].shape, pieces[0][1].dtype)
    for index, part in pieces:
        out = lax.dynamic_update_index_in_dim(out, part, index, 0)
    return out


def scatter_sum(lay, here, partial):
    s = lay.size
    low = partial.astype(jnp.bfloat16)
    kept = lax.dynamic_index_in_dim(low, here["c"], 1, keepdims=False)
    if s["c"] > 1:
        total = kept.astype(jnp.float32)
        for step in range(1, s["c"]):
            part = lax.dynamic_index_in_dim(low, (here["c"] + step) % s["c"], 1, keepdims=False)
            total = total + lay.send(part, c=step).astype(jnp.float32)
        kept = total.astype(jnp.bfloat16)
    total = pick(pick(kept, here["zl"]), here["x"]).astype(jnp.float32)
    for dl in range(s["zl"]):
        for dx in range(s["x"]):
            if dl == 0 and dx == 0:
                continue
            part = pick(
                pick(kept, (here["zl"] + dl) % s["zl"]), (here["x"] + dx) % s["x"]
            )
            total = total + lay.send(part, zl=dl, x=dx).astype(jnp.float32)
    return total


def gather_quad(lay, here, own):
    s = lay.size
    out = jnp.zeros((s["zl"], s["x"]) + own.shape, own.dtype)
    zeros = (0,) * own.ndim
    out = lax.dynamic_update_slice(out, own[None, None], (here["zl"], here["x"]) + zeros)
    for dl in range(s["zl"]):
        for dx in range(s["x"]):
            if dl == 0 and dx == 0:
                continue
            got = lay.send(own, zl=dl, x=dx)
            where = (lay.back(here, "zl", dl), lay.back(here, "x", dx))
            out = lax.dynamic_update_slice(out, got[None, None], where + zeros)
    full = jnp.zeros((s["zl"], s["c"]) + out.shape[1:], own.dtype)
    full = lax.dynamic_update_index_in_dim(full, out, here["c"], 1)
    for step in range(1, s["c"]):
        got = lay.send(out, c=step)
        full = lax.dynamic_update_index_in_dim(full, got, lay.back(here, "c", step), 1)
    return full


def post_norm(residual, branch, gain, shift):
    summed = RESIDUAL_SCALE * residual.astype(jnp.float32) + branch
    average = jnp.mean(summed, -1, keepdims=True)
    mean_square = jnp.mean(summed * summed, -1, keepdims=True)
    variance = mean_square - average * average
    return ((summed - average) * lax.rsqrt(variance + EPSILON) * gain + shift).astype(jnp.bfloat16)


def layer(
    lay,
    tokens,
    gate_weight,
    up_weight,
    down_weight,
    gate_scale,
    up_scale,
    down_scale,
    bgate_weight,
    cgate_weight,
    value_weight,
    bgate_scale,
    cgate_scale,
    value_scale,
    conv_taps,
    mixout_weight,
    mixout_scale,
    first_gain,
    first_shift,
    mixer_gain,
    mixer_shift,
    last_gain,
    last_shift,
):
    s = lay.size
    here = lay.here()
    nl = s["zl"]
    tp_index = here["x"] * s["c"] + here["c"]
    rows, features = tokens.shape
    width = features * lay.tp
    chunk = rows // lay.tp
    low = lambda w: w.astype(jnp.bfloat16)
    col_halves = lambda w: [low(h) for h in jnp.split(w, nl, axis=1)]

    gu = jnp.stack(
        [
            jnp.concatenate([g, u], axis=1)
            for g, u in zip(col_halves(gate_weight), col_halves(up_weight))
        ]
    )
    hid = gate_weight.shape[1] // nl
    dn = low(down_weight).reshape(nl, hid, -1)
    bcv = jnp.stack(
        [
            jnp.concatenate(p, axis=1)
            for p in zip(
                col_halves(bgate_weight), col_halves(cgate_weight), col_halves(value_weight)
            )
        ]
    )
    ch = bgate_weight.shape[1] // nl
    mo = low(mixout_weight).reshape(nl, ch, -1)

    gu_all = assemble(gather_pieces(lay, here, gu), lay.fs).reshape(width, 2 * hid)
    dn_all = assemble(gather_pieces(lay, here, dn), lay.fs)
    bcv_all = assemble(gather_pieces(lay, here, bcv), lay.fs).reshape(width, 3 * ch)
    mo_all = assemble(gather_pieces(lay, here, mo), lay.fs)

    names = [gate_scale, up_scale, bgate_scale, cgate_scale, value_scale, down_scale, mixout_scale]
    sizes = [n.shape[1] for n in names]
    packed = gather_small(lay, here, jnp.concatenate([n[0] for n in names]))
    cuts, at = [], 0
    for size in sizes:
        cuts.append(packed[:, :, at : at + size])
        at += size

    def own_cols(cut):
        cols = lax.dynamic_index_in_dim(cut, tp_index, 1, keepdims=False).reshape(nl, -1)
        return pick(cols, here["zl"])

    def all_cols(cut):
        return cut.transpose(1, 0, 2).reshape(-1)

    gate_cols, up_cols, b_cols, c_cols, v_cols = [own_cols(cut) for cut in cuts[:5]]
    down_cols, mixout_cols = [all_cols(cut) for cut in cuts[5:]]

    def blocks_dot(left, blocks):
        parts = [
            jnp.dot(left, blocks[i], preferred_element_type=jnp.float32)
            for i in range(blocks.shape[0])
        ]
        return jnp.concatenate(parts, axis=1)

    def hidden_of(v):
        both = jnp.dot(v, gu_all, preferred_element_type=jnp.float32)
        gate_sum, up_sum = both[:, :hid] * gate_cols, both[:, hid:] * up_cols
        return low(jax.nn.silu(gate_sum) * up_sum)

    def by_owner(partial):
        return partial.reshape(nl, s["c"], s["x"], chunk, -1)

    def feed_partial(v):
        return blocks_dot(hidden_of(v), dn_all)

    got = gather_quad(lay, here, tokens)
    v = got.transpose(0, 3, 2, 1, 4).reshape(nl * rows, width)
    mine = (here["zl"] * s["c"] + here["c"]) * s["x"] + here["x"]
    residual = lax.dynamic_slice_in_dim(v, mine * chunk, chunk, 0)

    branch = HALF_STEP * (scatter_sum(lay, here, by_owner(feed_partial(v))) * down_cols)
    first = post_norm(residual, branch, first_gain, first_shift)
    v = gather_quad(lay, here, first).reshape(nl * rows, width)

    three = jnp.dot(v, bcv_all, preferred_element_type=jnp.float32)
    outgate, ingate, values = [three[:, i * ch : (i + 1) * ch] for i in range(3)]
    taps = lax.dynamic_slice_in_dim(conv_taps, (tp_index * nl + here["zl"]) * ch, ch, 1)
    mixed = (ingate * c_cols * (values * v_cols)).reshape(-1, LENGTH, ch)
    padded = jnp.pad(mixed, ((0, 0), (TAPS - 1, 0), (0, 0)))
    convolved = jnp.zeros(mixed.shape, jnp.float32)
    for k in range(TAPS):
        convolved = convolved + taps[k] * padded[:, k : k + LENGTH]
    gated = low(outgate * b_cols * convolved.reshape(-1, ch))
    branch = scatter_sum(lay, here, by_owner(blocks_dot(gated, mo_all))) * mixout_cols
    second = post_norm(first, branch, mixer_gain, mixer_shift)
    v = gather_quad(lay, here, second).reshape(nl * rows, width)

    branch = HALF_STEP * (scatter_sum(lay, here, by_owner(feed_partial(v))) * down_cols)
    last = post_norm(second, branch, last_gain, last_shift)

    parts = last.reshape(chunk, lay.tp, features)
    out = jnp.zeros((s["c"], s["x"], chunk, features), last.dtype)
    for dx in range(s["x"]):
        for dc in range(s["c"]):
            to = ((here["x"] + dx) % s["x"]) * s["c"] + (here["c"] + dc) % s["c"]
            part = lax.dynamic_index_in_dim(parts, to, 1, keepdims=False)
            if dx or dc:
                part = lay.send(part, x=dx, c=dc)
            where = (lay.back(here, "c", dc), lay.back(here, "x", dx), 0, 0)
            out = lax.dynamic_update_slice(out, part[None, None], where)
    return out.reshape(rows, features)


def solution(mesh):
    lay = Layout(mesh)
    in_specs = (
        (P("fs", "tp"),) * 3
        + (P("tp", "fs"),) * 4
        + (P("fs", "tp"),) * 3
        + (P("tp", "fs"),) * 3
        + (P(),)
        + (P("tp", "fs"),) * 2
        + (P(),) * 6
    )

    def shards(*args):
        return layer(lay, *args)

    return jax.shard_map(
        shards, mesh=mesh, in_specs=in_specs, out_specs=P("fs", "tp"), check_vma=False
    )
```
